32 devices in a mesh: sp: 8 (over z, y), tp: 4 (over x, core).
Axes of the slice: x: 2, y: 2, z: 4, core: 2. Of those that a mesh axis runs over, the one named last changes fastest.
Arguments:
- residual: bfloat16 [8192, 2048], P('sp'), may hold values from -8 to 8
- query_wide: bfloat16 [8192, 1024], P('sp', 'tp'), may hold values from -6 to 6
- key_wide: bfloat16 [8192, 1024], P('sp', 'tp'), may hold values from -6 to 6
- value_wide: bfloat16 [8192, 2048], P('sp', 'tp'), may hold values from -6 to 6
- decay_wide: bfloat16 [8192, 1024], P('sp', 'tp'), may hold values from -12 to 12
- gate_wide: bfloat16 [8192, 2048], P('sp', 'tp'), may hold values from -6 to 6
- query_narrow: bfloat16 [8192, 512], P('sp', 'tp'), may hold values from -6 to 6
- key_narrow: bfloat16 [8192, 512], P('sp', 'tp'), may hold values from -6 to 6
- value_narrow: bfloat16 [8192, 2048], P('sp', 'tp'), may hold values from -6 to 6
- decay_narrow: bfloat16 [8192, 512], P('sp', 'tp'), may hold values from -12 to 12
- gate_narrow: bfloat16 [8192, 2048], P('sp', 'tp'), may hold values from -6 to 6
- head_gain: float32 [512], replicated, may hold values from 0.1 to 1.9
- out_wide: bfloat16 [2048, 2048], P('tp'), may hold values from -0.125 to 0.125
- out_narrow: bfloat16 [2048, 2048], P('tp'), may hold values from -0.125 to 0.125
- mlp_gain: float32 [2048], replicated, may hold values from 0.1 to 1.9
- up_weight: bfloat16 [2048, 4096], P('sp', 'tp'), may hold values from -0.125 to 0.125
- down_weight: bfloat16 [4096, 2048], P('tp', 'sp'), may hold values from -0.09375 to 0.09375
Outputs:
- layer_out: bfloat16 [8192, 2048], P('sp', 'tp')
The draws below stay inside these ranges and needn't reach their ends.
All inputs are finite; a program needn't handle non-finite values.
Results may differ from the reference program's by a relative error of at most 0.017.
Values may be sent and summed in bfloat16 or wider, within the bound.
A program may use at most 128 MiB of HBM per device.

```python
import math
import jax
import jax.numpy as jnp
from jax import lax

D = 2048
FF = 4096
HEADS = 4
HEAD_KA = 256
HEAD_KB = 128
HEAD_V = 512
BLOCK = 64
TOK_DEV = 1024
SEQUENCE_TOKENS = 8192
N_TP = 4


def draw_residual(key, part):
    column = jnp.arange(D, dtype=jnp.float32) / D
    baseline = jax.random.normal(jax.random.fold_in(key, 3), (SEQUENCE_TOKENS, D), jnp.float32)
    scale = 0.5 * jnp.power(4.0, column)
    return jnp.clip(baseline * scale[None, :], -8.0, 8.0).astype(jnp.bfloat16)


def decay_draw(key, head_width, salt):
    random_subkeys = jax.random.split(jax.random.fold_in(key, salt), 6)
    channel_count = HEADS * head_width
    ranking = jax.random.permutation(random_subkeys[0], HEADS)
    slow_heads = ranking < HEADS // 2
    jitter = jnp.clip(jax.random.normal(random_subkeys[1], (SEQUENCE_TOKENS, channel_count), jnp.float32), -3.0, 3.0)
    offsets = jax.random.uniform(random_subkeys[2], (SEQUENCE_TOKENS // TOK_DEV,), jnp.float32, -0.7, 0.7)
    slow_cols = jnp.repeat(slow_heads, head_width, total_repeat_length=channel_count)
    baseline = jnp.where(slow_cols, math.log(SEQUENCE_TOKENS / 4.0), 1.0)
    spread = jax.random.uniform(random_subkeys[3], (channel_count,), jnp.float32, -0.5, 0.5)
    grouped_rows = jax.random.randint(random_subkeys[4], (3,), 0, SEQUENCE_TOKENS)
    group_match = jnp.any(jnp.arange(SEQUENCE_TOKENS)[:, None] == grouped_rows[None, :], axis=1)
    group_depth = jax.random.uniform(random_subkeys[5], (SEQUENCE_TOKENS, 1), jnp.float32, 3.5, 8.0)
    row_offsets = jnp.repeat(offsets, TOK_DEV, total_repeat_length=SEQUENCE_TOKENS)
    before_activation = baseline[None, :] + spread[None, :] + row_offsets[:, None] + jitter
    before_activation = jnp.where(group_match[:, None], -group_depth, before_activation)
    return jnp.clip(before_activation, -12.0, 12.0).astype(jnp.bfloat16)


def draw_decay_wide(key, part):
    return decay_draw(key, HEAD_KA, 11)


def draw_decay_narrow(key, part):
    return decay_draw(key, HEAD_KB, 13)


def levels(rng, extent, pieces, least, largest):
    def one(dim, blocks):
        draws = jax.random.uniform(jax.random.fold_in(jax.random.fold_in(rng, 6), dim), (blocks,), jnp.float32, least / len(pieces), largest / len(pieces))
        return jnp.repeat(jnp.exp(draws), extent[dim] // blocks).reshape((-1,) + (1,) * (len(extent) - dim - 1))

    factor_of = one(*pieces[0])
    for cut in pieces[1:]:
        factor_of = factor_of * one(*cut)
    return factor_of


def centred(own_key, extent, scale, bound, pieces=(), kind=jnp.bfloat16):
    gain = levels(own_key, extent, pieces, -0.22, 0.18) if pieces else 1.0
    drawn = jax.random.normal(own_key, extent, jnp.float32) * scale * gain
    return jnp.minimum(jnp.maximum(drawn, -bound), bound).astype(kind)


def setup_inputs(seed: int = 0) -> dict:
    streams_of = jax.random.split(jax.random.key(seed), 18)
    residual = draw_residual(jax.random.fold_in(streams_of[17], 71), 0)
    query_wide = centred(streams_of[1], (SEQUENCE_TOKENS, HEADS * HEAD_KA), 1.0, 6.0, ((0, 8), (1, 4)))
    key_wide = centred(streams_of[2], (SEQUENCE_TOKENS, HEADS * HEAD_KA), 1.0, 6.0, ((0, 8), (1, 4)))
    value_wide = centred(streams_of[3], (SEQUENCE_TOKENS, HEADS * HEAD_V), 1.0, 6.0, ((0, 8), (1, 4)))
    decay_wide = draw_decay_wide(jax.random.fold_in(streams_of[17], 71), 0)
    gate_wide = centred(streams_of[5], (SEQUENCE_TOKENS, HEADS * HEAD_V), 1.0, 6.0, ((0, 8), (1, 4)))
    query_narrow = centred(streams_of[6], (SEQUENCE_TOKENS, HEADS * HEAD_KB), 1.0, 6.0, ((0, 8), (1, 4)))
    key_narrow = centred(streams_of[7], (SEQUENCE_TOKENS, HEADS * HEAD_KB), 1.0, 6.0, ((0, 8), (1, 4)))
    value_narrow = centred(streams_of[8], (SEQUENCE_TOKENS, HEADS * HEAD_V), 1.0, 6.0, ((0, 8), (1, 4)))
    decay_narrow = draw_decay_narrow(jax.random.fold_in(streams_of[17], 71), 0)
    gate_narrow = centred(streams_of[10], (SEQUENCE_TOKENS, HEADS * HEAD_V), 1.0, 6.0, ((0, 8), (1, 4)))
    head_gain = jnp.clip(1.0 + 0.18 * jax.random.normal(streams_of[11], (HEAD_V,), jnp.float32), 0.1, 1.9)
    out_wide = centred(streams_of[12], (HEADS * HEAD_V, D), (HEADS * HEAD_V) ** -0.5, 0.125, ((0, 4),))
    out_narrow = centred(streams_of[13], (HEADS * HEAD_V, D), (HEADS * HEAD_V) ** -0.5, 0.125, ((0, 4),))
    mlp_gain = jnp.clip(1.0 + 0.18 * jax.random.normal(streams_of[14], (D,), jnp.float32), 0.1, 1.9)
    up_weight = centred(streams_of[15], (D, FF), D ** -0.5, 0.125, ((0, 8), (1, 4)))
    down_weight = centred(streams_of[16], (FF, D), FF ** -0.5, 0.09375, ((0, 4), (1, 8)))
    return dict(residual=residual, query_wide=query_wide, key_wide=key_wide, value_wide=value_wide, decay_wide=decay_wide, gate_wide=gate_wide, query_narrow=query_narrow, key_narrow=key_narrow, value_narrow=value_narrow, decay_narrow=decay_narrow, gate_narrow=gate_narrow, head_gain=head_gain, out_wide=out_wide, out_narrow=out_narrow, mlp_gain=mlp_gain, up_weight=up_weight, down_weight=down_weight)


EPS = 1e-05
DECAY_NORMALIZER = 16.0
HIGHEST = lax.Precision.HIGHEST

def block_pass(queries, keys_in, values_in, log_decay, block_len):
    num_blocks = queries.shape[0] // block_len

    def to_blocks(stacked):
        return stacked.reshape((num_blocks, block_len) + stacked.shape[1:])
    causal = jnp.tril(jnp.ones((block_len, block_len), dtype=bool))
    initial = (jnp.zeros((queries.shape[1], queries.shape[2], values_in.shape[2]), jnp.float32), jnp.zeros((queries.shape[1], queries.shape[2]), jnp.float32))

    def advance(running, inputs):
        memory, offset = running
        block_q, block_k, block_v, block_g = inputs
        within = jnp.cumsum(block_g, axis=0)
        final_log = within[-1]
        scaled_q = block_q * jnp.exp(within)
        scaled_k = block_k * jnp.exp(-within)
        outside = jnp.einsum('ihd,hde->ihe', scaled_q, memory, precision=HIGHEST)
        scores = jnp.einsum('ihd,jhd->hij', scaled_q, scaled_k, precision=HIGHEST)
        scores = jnp.where(causal[None], scores, 0.0)
        inside = jnp.einsum('hij,jhe->ihe', scores, block_v, precision=HIGHEST)
        decayed_keys = scaled_k * jnp.exp(final_log)[None]
        memory = jnp.exp(final_log)[..., None] * memory + jnp.einsum('jhd,jhe->hde', decayed_keys, block_v, precision=HIGHEST)
        carried_q = scaled_q * jnp.exp(offset)[None]
        return ((memory, offset + final_log), (outside + inside, carried_q))
    (memory, totals), (outputs, carried_q) = lax.scan(advance, initial, (to_blocks(queries), to_blocks(keys_in), to_blocks(values_in), to_blocks(log_decay)))
    return (outputs.reshape(values_in.shape), carried_q.reshape(queries.shape), totals, memory)

def prepare(query, key_proj, value, decay, heads_here):
    row_count = query.shape[0]
    key_width = query.shape[1] // heads_here
    queries = query.astype(jnp.float32).reshape(row_count, heads_here, key_width) * key_width ** (-0.5)
    keys_in = key_proj.astype(jnp.float32).reshape(row_count, heads_here, key_width)
    values_in = value.astype(jnp.float32).reshape(row_count, heads_here, value.shape[1] // heads_here)
    log_decay = jax.nn.log_sigmoid(decay.astype(jnp.float32)).reshape(row_count, heads_here, key_width) / DECAY_NORMALIZER
    return (queries, keys_in, values_in, log_decay)

def finish(outputs, gate, head_gain):
    scale = lax.rsqrt(lax.optimization_barrier(jnp.mean(jnp.square(outputs), axis=-1, keepdims=True)) + EPS)
    gated = outputs * scale * head_gain * jax.nn.silu(gate.astype(jnp.float32).reshape(outputs.shape))
    return gated.reshape(outputs.shape[0], -1).astype(jnp.bfloat16)

def group_output(query, key_proj, value, decay, gate, head_gain):
    queries, keys_in, values_in, log_decay = prepare(query, key_proj, value, decay, HEADS)
    outputs = block_pass(queries, keys_in, values_in, log_decay, BLOCK)[0]
    return finish(outputs, gate, head_gain)

def blockwise_sum(left_sides, right_sides):
    total = jnp.zeros((left_sides[0].shape[0], right_sides[0].shape[1]), jnp.float32)
    for tp_block in range(N_TP):
        block_sum = jnp.zeros_like(total)
        for left_side, right_side in zip(left_sides, right_sides):
            block_width = left_side.shape[1] // N_TP
            first_col = tp_block * block_width
            block_sum = block_sum + jnp.dot(left_side[:, first_col:first_col + block_width], right_side[first_col:first_col + block_width], preferred_element_type=jnp.float32)
        total = total + lax.optimization_barrier(block_sum.astype(jnp.bfloat16)).astype(jnp.float32)
    return total

def reference(residual, query_wide, key_wide, value_wide, decay_wide, gate_wide, query_narrow, key_narrow, value_narrow, decay_narrow, gate_narrow, head_gain, out_wide, out_narrow, mlp_gain, up_weight, down_weight):
    gated_wide = group_output(query_wide, key_wide, value_wide, decay_wide, gate_wide, head_gain)
    gated_narrow = group_output(query_narrow, key_narrow, value_narrow, decay_narrow, gate_narrow, head_gain)
    mixed = blockwise_sum((gated_wide, gated_narrow), (out_wide, out_narrow))
    stream = (residual.astype(jnp.float32) + mixed).astype(jnp.bfloat16)
    stream_f = stream.astype(jnp.float32)
    normed = (stream_f * lax.rsqrt(lax.optimization_barrier(jnp.mean(jnp.square(stream_f), axis=1, keepdims=True)) + EPS) * mlp_gain).astype(jnp.bfloat16)
    hidden = jnp.square(jax.nn.relu(jnp.dot(normed, up_weight, preferred_element_type=jnp.float32))).astype(jnp.bfloat16)
    mlp_sum = blockwise_sum((hidden,), (down_weight,))
    return (stream_f + mlp_sum).astype(jnp.bfloat16)
```

```python
import functools
import jax
import jax.numpy as jnp
from jax import lax
from jax.experimental import pallas as pl
from jax.experimental.pallas import tpu as pltpu
from jax.sharding import PartitionSpec as P

HEADS = 4
EPS = 1e-05
DECAY_NORMALIZER = 16.0
MESH = pl.DeviceIdType.MESH
BF = jnp.bfloat16
F32 = jnp.float32
VM = pltpu.VMEM


def vmem():
    return pl.BlockSpec(memory_space=VM)


def dot(a, b, dims):
    return lax.dot_general(a, b, (dims, ((), ())), preferred_element_type=F32)


NT = ((1,), (1,))
NN = ((1,), (0,))
TN = ((0,), (0,))


def local_group(q, k, v, d, out, carried, memory, offset, tril, scale):
    rows = q.shape[0]
    decay = d[...].astype(F32)
    g = (jnp.minimum(decay, 0.0) - jnp.log1p(jnp.exp(-jnp.abs(decay)))) / DECAY_NORMALIZER
    high = g.astype(BF)
    low = (g - high.astype(F32)).astype(BF)
    ones = tril.astype(F32).astype(BF)
    within = dot(ones, high, NN) + dot(ones, low, NN)
    mid = within[rows // 2 - 1 : rows // 2]
    last = within[rows - 1 : rows]
    scaled_q = q[...].astype(F32) * scale * jnp.exp(within - mid)
    scaled_k = k[...].astype(F32) * jnp.exp(mid - within)
    value = v[...]
    scores = dot(scaled_q.astype(BF), scaled_k.astype(BF), NT)
    scores = jnp.where(tril, scores, 0.0).astype(BF)
    whole_q = scaled_q * jnp.exp(mid)
    state = memory[...]
    out[...] = (dot(scores, value, NN) + dot(whole_q.astype(BF), state.astype(BF), NT)).astype(
        out.dtype
    )
    carried[...] = (whole_q * jnp.exp(offset[...])).astype(BF)
    keys = (scaled_k * jnp.exp(last - mid)).astype(BF)
    memory[...] = state * jnp.exp(last) + dot(value, keys, TN)
    offset[...] = offset[...] + last


def local_kernel(
    qw, kw, vw, dw, qn, kn, vn, dn, ow, cw, on, cn, packed, mw, mn, fw, fn
):
    step = pl.program_id(0)
    rows = qw.shape[0]

    @pl.when(step == 0)
    def _():
        for ref in (mw, mn, fw, fn):
            ref[...] = jnp.zeros_like(ref)

    tril = lax.broadcasted_iota(jnp.int32, (rows, rows), 0) >= lax.broadcasted_iota(
        jnp.int32, (rows, rows), 1
    )
    local_group(qw, kw, vw, dw, ow, cw, mw, fw, tril, qw.shape[1] ** -0.5)
    local_group(qn, kn, vn, dn, on, cn, mn, fn, tril, qn.shape[1] ** -0.5)

    @pl.when(step == pl.num_programs(0) - 1)
    def _():
        wide, values = qw.shape[1], vw.shape[1]
        packed[:values, :wide] = mw[...].astype(BF)
        packed[:values, wide:] = mn[...].astype(BF)
        extra = packed.shape[0] - values
        packed[values:, :wide] = jnp.broadcast_to(jnp.exp(fw[...]), (extra, wide)).astype(BF)
        packed[values:, wide:] = jnp.broadcast_to(
            jnp.exp(fn[...]), (extra, qn.shape[1])
        ).astype(BF)


def local_pass(qw, kw, vw, dw, qn, kn, vn, dn):
    tokens, wide = qw.shape
    narrow, values = qn.shape[1], vw.shape[1]
    rows = min(128, tokens)

    def spec(width):
        return pl.BlockSpec((rows, width), lambda i: (i, 0))

    whole = (values + 16, wide + narrow)
    return pl.pallas_call(
        local_kernel,
        grid=(tokens // rows,),
        in_specs=[spec(x.shape[1]) for x in (qw, kw, vw, dw, qn, kn, vn, dn)],
        out_specs=[
            spec(values), spec(wide), spec(values), spec(narrow),
            pl.BlockSpec(whole, lambda i: (0, 0)),
        ],
        out_shape=[
            jax.ShapeDtypeStruct((tokens, values), BF),
            jax.ShapeDtypeStruct((tokens, wide), BF),
            jax.ShapeDtypeStruct((tokens, values), BF),
            jax.ShapeDtypeStruct((tokens, narrow), BF),
            jax.ShapeDtypeStruct(whole, BF),
        ],
        scratch_shapes=[
            VM((values, wide), F32), VM((values, narrow), F32),
            VM((1, wide), F32), VM((1, narrow), F32),
        ],
        cost_estimate=pl.CostEstimate(
            flops=30 * 10**9, bytes_accessed=12 * 2**20, transcendentals=0
        ),
        name="local_pass",
    )(qw, kw, vw, dw, qn, kn, vn, dn)


def ring_kernel(n, mine, every, send_sem, recv_sem):
    s = lax.axis_index("sp")
    half = n // 2

    def index_of(p):
        p = lax.rem(p + n, n)
        return jnp.where(p < half, 2 * p, 2 * (n - 1 - p) + 1)

    place = jnp.where(lax.rem(s, 2) == 0, s // 2, n - (s + 1) // 2)
    sides = (index_of(place + 1), index_of(place - 1))
    barrier = pltpu.get_barrier_semaphore()
    for side in sides:
        pl.semaphore_signal(barrier, inc=1, device_id={"sp": side}, device_id_type=MESH)
    pl.semaphore_wait(barrier, 2)
    cut = mine.shape[0] // 32 * 16
    pieces = (pl.ds(0, cut), pl.ds(cut, mine.shape[0] - cut))
    copies = {}
    for far in range(1, half + 1):
        for piece in (0, 1):
            for way in (0, 1):
                if far == half and piece != way:
                    continue
                origin = index_of(place - (far - 1) if way == 0 else place + (far - 1))
                if far > 1:
                    copies[far - 1, piece, way].wait_recv()
                    source = every.at[origin, pieces[piece]]
                else:
                    source = mine.at[pieces[piece]]
                copy = pltpu.make_async_remote_copy(
                    src_ref=source,
                    dst_ref=every.at[origin, pieces[piece]],
                    send_sem=send_sem.at[way, far - 1, piece],
                    recv_sem=recv_sem.at[way, far - 1, piece],
                    device_id={"sp": sides[way]},
                    device_id_type=MESH,
                )
                copy.start()
                copies[far, piece, way] = copy
    every[s] = mine[...]
    for (far, piece, way), copy in copies.items():
        copy.wait_send()
        if far == half or (far == half - 1 and piece != way):
            copy.wait_recv()


def ring(packed, n):
    return pl.pallas_call(
        functools.partial(ring_kernel, n),
        out_shape=jax.ShapeDtypeStruct((n,) + packed.shape, BF),
        in_specs=[vmem()],
        out_specs=vmem(),
        scratch_shapes=[
            pltpu.SemaphoreType.DMA((2, n // 2, 2)),
            pltpu.SemaphoreType.DMA((2, n // 2, 2)),
        ],
        compiler_params=pltpu.CompilerParams(collective_id=0, has_side_effects=True),
        cost_estimate=pl.CostEstimate(
            flops=30 * 10**9, bytes_accessed=2**20, transcendentals=0
        ),
        name="state_ring",
    )(packed)


def gated(local, carried, state, gate, gain):
    out = local[...].astype(F32) + dot(carried[...], state, NT)
    scale = lax.rsqrt(jnp.mean(jnp.square(out), axis=-1, keepdims=True) + EPS)
    u = gate[...].astype(F32)
    return (out * scale * gain[...] * (u / (1.0 + jnp.exp(-u)))).astype(BF)


def finish_kernel(every, ow, cw, gw, on, cn, gn, gain, weight_w, weight_n, out, total, state):
    wide = cw.shape[1]
    values = ow.shape[1]

    @pl.when(pl.program_id(0) == 0)
    def _():
        total[...] = jnp.zeros_like(total)

        def one(j, carry):
            decay = every[j, values : values + 16, :].astype(F32)[:1]
            total[...] = total[...] * decay + every[j, :values, :].astype(F32)
            return carry

        lax.fori_loop(0, lax.axis_index("sp"), one, 0)
        state[...] = total[...].astype(BF)

    left = gated(ow, cw, state[:, :wide], gw, gain)
    right = gated(on, cn, state[:, wide:], gn, gain)
    out[...] = (dot(left, weight_w[...], NN) + dot(right, weight_n[...], NN)).astype(BF)


def finish(every, ow, cw, gw, on, cn, gn, gain, weight_w, weight_n):
    tokens, values = ow.shape
    rows = min(256, tokens)
    width = weight_w.shape[1]

    def spec(x):
        return pl.BlockSpec((rows, x.shape[1]), lambda i: (i, 0))

    return pl.pallas_call(
        finish_kernel,
        grid=(tokens // rows,),
        in_specs=[vmem()]
        + [spec(x) for x in (ow, cw, gw, on, cn, gn)]
        + [vmem()] * 3,
        out_specs=pl.BlockSpec((rows, width), lambda i: (i, 0)),
        out_shape=jax.ShapeDtypeStruct((tokens, width), BF),
        scratch_shapes=[
            VM((values, every.shape[2]), F32),
            VM((values, every.shape[2]), BF),
        ],
        compiler_params=pltpu.CompilerParams(vmem_limit_bytes=48 * 2**20),
        cost_estimate=pl.CostEstimate(
            flops=20 * 10**9, bytes_accessed=16 * 2**20, transcendentals=0
        ),
        name="finish",
    )(every, ow, cw, gw, on, cn, gn, gain.reshape(1, -1), weight_w, weight_n)


def remote(src, dst, send, recv, to):
    copy = pltpu.make_async_remote_copy(
        src_ref=src, dst_ref=dst, send_sem=send, recv_sem=recv,
        device_id={"tp": to}, device_id_type=MESH,
    )
    copy.start()
    return copy


def greet(t):
    barrier = pltpu.get_barrier_semaphore()
    near, far = t + 1 - 2 * lax.rem(t, 2), lax.rem(t + 2, 4)
    for other in (near, far):
        pl.semaphore_signal(barrier, inc=1, device_id={"tp": other}, device_id_type=MESH)
    pl.semaphore_wait(barrier, 2)
    return near, far, lax.rem(near + 2, 4)


def reduce_steps(block, chunks, t, near, far, cross, partial, r1, mix, r2, sems, use):
    s1, v1, s2, v2 = sems
    rows = mix.shape[1]
    sent = []
    for which, owner in ((1, cross), (0, near)):
        for c in range(chunks):
            sent.append(
                (which, c, remote(
                    partial.at[block(owner, c)], r1.at[which, c],
                    s1.at[which, c], v1.at[which, c], near,
                ))
            )
    first = {(w, c): x for w, c, x in sent}
    second = []
    for c in range(chunks):
        first[1, c].wait_recv()
        mix[c] = (partial[block(far, c)].astype(F32) + r1[1, c].astype(F32)).astype(BF)
        second.append(remote(mix.at[c], r2.at[c], s2.at[c], v2.at[c], far))
    for c in range(chunks):
        first[0, c].wait_recv()
        second[c].wait_recv()
        use(c, partial[block(t, c)].astype(F32) + r1[0, c].astype(F32) + r2[c].astype(F32))
    return [x for _, _, x in sent] + second


def mix_kernel(
    chunks, partial, residual, gain, stream, normed,
    r1, mix, r2, s1, v1, s2, v2, sx, vx, sn, vn, sf, vf,
):
    t = lax.axis_index("tp")
    near, far, cross = greet(t)
    rows = mix.shape[1]
    own = rows * chunks

    def block(owner, c):
        return pl.ds(pl.multiple_of(owner * own + c * rows, rows), rows), slice(None)

    def norm(where):
        x = stream[where].astype(F32)
        scale = lax.rsqrt(jnp.mean(jnp.square(x), axis=1, keepdims=True) + EPS)
        normed[where] = (x * scale * gain[...]).astype(BF)

    across, beside, relayed = [], [], []

    def use(c, value):
        where = block(t, c)
        stream[where] = (residual[pl.ds(c * rows, rows), :].astype(F32) + value).astype(BF)
        across.append(remote(stream.at[where], stream.at[where], sx.at[c], vx.at[c], far))
        beside.append(remote(stream.at[where], stream.at[where], sn.at[c], vn.at[c], near))

    started = reduce_steps(
        block, chunks, t, near, far, cross, partial, r1, mix, r2, (s1, v1, s2, v2), use
    )
    for c in range(chunks):
        norm(block(t, c))
        beside[c].wait_recv()
        norm(block(near, c))
    for c in range(chunks):
        across[c].wait_recv()
        where = block(far, c)
        relayed.append(remote(stream.at[where], stream.at[where], sf.at[c], vf.at[c], near))
        norm(where)
    for c in range(chunks):
        relayed[c].wait_recv()
        norm(block(cross, c))
    for copy in started + across + beside + relayed:
        copy.wait_send()


def mix_rows(partial, residual, gain):
    tokens, width = partial.shape
    chunks = 4
    rows = tokens // 4 // chunks
    dma = pltpu.SemaphoreType.DMA
    return pl.pallas_call(
        functools.partial(mix_kernel, chunks),
        out_shape=[jax.ShapeDtypeStruct((tokens, width), BF)] * 2,
        in_specs=[vmem()] * 3,
        out_specs=[vmem()] * 2,
        scratch_shapes=[
            VM((2, chunks, rows, width), BF), VM((chunks, rows, width), BF),
            VM((chunks, rows, width), BF),
            dma((2, chunks)), dma((2, chunks)),
        ] + [dma((chunks,))] * 8,
        compiler_params=pltpu.CompilerParams(
            collective_id=1, has_side_effects=True, vmem_limit_bytes=48 * 2**20
        ),
        cost_estimate=pl.CostEstimate(
            flops=50 * 10**9, bytes_accessed=16 * 2**20, transcendentals=0
        ),
        name="mix_rows",
    )(partial, residual, gain.reshape(1, -1))


def last_kernel(chunks, partial, stream, out, r1, mix, r2, s1, v1, s2, v2):
    t = lax.axis_index("tp")
    near, far, cross = greet(t)
    rows, width = mix.shape[1:]

    def block(owner, c):
        return pl.ds(c * rows, rows), pl.ds(pl.multiple_of(owner * width, width), width)

    def use(c, value):
        where = pl.ds(c * rows, rows)
        out[where, :] = (stream[where, :].astype(F32) + value).astype(BF)

    for copy in reduce_steps(
        block, chunks, t, near, far, cross, partial, r1, mix, r2, (s1, v1, s2, v2), use
    ):
        copy.wait_send()


def last_columns(partial, stream):
    tokens, width = stream.shape
    chunks = 4
    rows = tokens // chunks
    dma = pltpu.SemaphoreType.DMA
    return pl.pallas_call(
        functools.partial(last_kernel, chunks),
        out_shape=jax.ShapeDtypeStruct((tokens, width), BF),
        in_specs=[vmem()] * 2,
        out_specs=vmem(),
        scratch_shapes=[
            VM((2, chunks, rows, width), BF), VM((chunks, rows, width), BF),
            VM((chunks, rows, width), BF),
            dma((2, chunks)), dma((2, chunks)), dma((chunks,)), dma((chunks,)),
        ],
        compiler_params=pltpu.CompilerParams(
            collective_id=2, has_side_effects=True, vmem_limit_bytes=32 * 2**20
        ),
        name="last_columns",
    )(partial, stream)


def body(
    residual,
    query_wide,
    key_wide,
    value_wide,
    decay_wide,
    gate_wide,
    query_narrow,
    key_narrow,
    value_narrow,
    decay_narrow,
    gate_narrow,
    head_gain,
    out_wide,
    out_narrow,
    mlp_gain,
    up_weight,
    down_weight,
):
    n_sp, n_tp = lax.axis_size("sp"), lax.axis_size("tp")
    assert n_tp == HEADS == 4 and n_sp % 2 == 0
    up_whole = lax.all_gather(up_weight, "sp", axis=0, tiled=True)
    down_whole = lax.all_gather(down_weight, "sp", axis=1, tiled=True)
    wide_out, wide_q, narrow_out, narrow_q, packed = local_pass(
        query_wide, key_wide, value_wide, decay_wide,
        query_narrow, key_narrow, value_narrow, decay_narrow,
    )
    every = ring(packed, n_sp)
    partial = finish(
        every, wide_out, wide_q, gate_wide, narrow_out, narrow_q, gate_narrow,
        head_gain, out_wide, out_narrow,
    )
    t = lax.axis_index("tp")
    own_rows = residual.shape[0] // n_tp
    own_cols = residual.shape[1] // n_tp
    residual_rows = lax.dynamic_slice_in_dim(residual, t * own_rows, own_rows, 0)
    stream, normed = mix_rows(partial, residual_rows, mlp_gain)
    stream_cols = lax.dynamic_slice_in_dim(stream, t * own_cols, own_cols, 1)
    before = jnp.dot(normed, up_whole, preferred_element_type=F32)
    hidden = jnp.square(jax.nn.relu(before)).astype(BF)
    down_terms = jnp.dot(hidden, down_whole, preferred_element_type=F32).astype(BF)
    return last_columns(down_terms, stream_cols)


def solution(mesh):
    return jax.shard_map(
        body,
        mesh=mesh,
        in_specs=(
            P("sp", None),
            P("sp", "tp"),
            P("sp", "tp"),
            P("sp", "tp"),
            P("sp", "tp"),
            P("sp", "tp"),
            P("sp", "tp"),
            P("sp", "tp"),
            P("sp", "tp"),
            P("sp", "tp"),
            P("sp", "tp"),
            P(),
            P("tp", None),
            P("tp", None),
            P(),
            P("sp", "tp"),
            P("tp", "sp"),
        ),
        out_specs=P("sp", "tp"),
        check_vma=False,
    )
```

```python
import functools
import jax
import jax.numpy as jnp
from jax import lax
from jax.experimental import pallas as pl
from jax.experimental.pallas import tpu as pltpu
from jax.sharding import PartitionSpec as P

HEADS = 4
EPS = 1e-05
DECAY_NORMALIZER = 16.0
MESH = pl.DeviceIdType.MESH
BF = jnp.bfloat16
F32 = jnp.float32
VM = pltpu.VMEM


def vmem():
    return pl.BlockSpec(memory_space=VM)


def dot(a, b, dims):
    return lax.dot_general(a, b, (dims, ((), ())), preferred_element_type=F32)


NT = ((1,), (1,))
NN = ((1,), (0,))
TN = ((0,), (0,))


def local_group(q, k, v, d, out, carried, memory, offset, tril, scale):
    rows = q.shape[0]
    decay = d[...].astype(F32)
    g = (jnp.minimum(decay, 0.0) - jnp.log1p(jnp.exp(-jnp.abs(decay)))) / DECAY_NORMALIZER
    high = g.astype(BF)
    low = (g - high.astype(F32)).astype(BF)
    ones = tril.astype(F32).astype(BF)
    within = dot(ones, high, NN) + dot(ones, low, NN)
    mid = within[rows // 2 - 1 : rows // 2]
    last = within[rows - 1 : rows]
    scaled_q = q[...].astype(F32) * scale * jnp.exp(within - mid)
    scaled_k = k[...].astype(F32) * jnp.exp(mid - within)
    value = v[...]
    scores = dot(scaled_q.astype(BF), scaled_k.astype(BF), NT)
    scores = jnp.where(tril, scores, 0.0).astype(BF)
    whole_q = scaled_q * jnp.exp(mid)
    state = memory[...]
    out[...] = (dot(scores, value, NN) + dot(whole_q.astype(BF), state.astype(BF), NT)).astype(
        out.dtype
    )
    carried[...] = (whole_q * jnp.exp(offset[...])).astype(BF)
    keys = (scaled_k * jnp.exp(last - mid)).astype(BF)
    memory[...] = state * jnp.exp(last) + dot(value, keys, TN)
    offset[...] = offset[...] + last


def local_kernel(
    qw, kw, vw, dw, qn, kn, vn, dn, ow, cw, on, cn, packed, mw, mn, fw, fn
):
    step = pl.program_id(0)
    rows = qw.shape[0]

    @pl.when(step == 0)
    def _():
        for ref in (mw, mn, fw, fn):
            ref[...] = jnp.zeros_like(ref)

    tril = lax.broadcasted_iota(jnp.int32, (rows, rows), 0) >= lax.broadcasted_iota(
        jnp.int32, (rows, rows), 1
    )
    local_group(qw, kw, vw, dw, ow, cw, mw, fw, tril, qw.shape[1] ** -0.5)
    local_group(qn, kn, vn, dn, on, cn, mn, fn, tril, qn.shape[1] ** -0.5)

    @pl.when(step == pl.num_programs(0) - 1)
    def _():
        wide, values = qw.shape[1], vw.shape[1]
        packed[:values, :wide] = mw[...].astype(BF)
        packed[:values, wide:] = mn[...].astype(BF)
        extra = packed.shape[0] - values
        packed[values:, :wide] = jnp.broadcast_to(jnp.exp(fw[...]), (extra, wide)).astype(BF)
        packed[values:, wide:] = jnp.broadcast_to(
            jnp.exp(fn[...]), (extra, qn.shape[1])
        ).astype(BF)


def local_pass(qw, kw, vw, dw, qn, kn, vn, dn):
    tokens, wide = qw.shape
    narrow, values = qn.shape[1], vw.shape[1]
    rows = min(128, tokens)

    def spec(width):
        return pl.BlockSpec((rows, width), lambda i: (i, 0))

    whole = (values + 16, wide + narrow)
    return pl.pallas_call(
        local_kernel,
        grid=(tokens // rows,),
        in_specs=[spec(x.shape[1]) for x in (qw, kw, vw, dw, qn, kn, vn, dn)],
        out_specs=[
            spec(values), spec(wide), spec(values), spec(narrow),
            pl.BlockSpec(whole, lambda i: (0, 0)),
        ],
        out_shape=[
            jax.ShapeDtypeStruct((tokens, values), BF),
            jax.ShapeDtypeStruct((tokens, wide), BF),
            jax.ShapeDtypeStruct((tokens, values), BF),
            jax.ShapeDtypeStruct((tokens, narrow), BF),
            jax.ShapeDtypeStruct(whole, BF),
        ],
        scratch_shapes=[
            VM((values, wide), F32), VM((values, narrow), F32),
            VM((1, wide), F32), VM((1, narrow), F32),
        ],
        cost_estimate=pl.CostEstimate(
            flops=30 * 10**9, bytes_accessed=12 * 2**20, transcendentals=0
        ),
        name="local_pass",
    )(qw, kw, vw, dw, qn, kn, vn, dn)


def ring_place(n):
    s = lax.axis_index("sp")
    half = n // 2

    def index_of(p):
        p = lax.rem(p + n, n)
        return jnp.where(p < half, 2 * p, 2 * (n - 1 - p) + 1)

    place = jnp.where(lax.rem(s, 2) == 0, s // 2, n - (s + 1) // 2)
    return place, index_of, (index_of(place + 1), index_of(place - 1))


def ring_steps(n, mine, every, send_sem, recv_sem):
    half = n // 2
    place, index_of, sides = ring_place(n)
    cut = mine.shape[0] // 32 * 16
    pieces = (pl.ds(0, cut), pl.ds(cut, mine.shape[0] - cut))
    copies = {}

    def hop(far, piece, way):
        origin = index_of(place - (far - 1) if way == 0 else place + (far - 1))
        if far > 1:
            copies[far - 1, piece, way].wait_recv()
            source = every.at[origin, pieces[piece]]
        else:
            source = mine.at[pieces[piece]]
        copy = pltpu.make_async_remote_copy(
            src_ref=source,
            dst_ref=every.at[origin, pieces[piece]],
            send_sem=send_sem.at[way, far - 1, piece],
            recv_sem=recv_sem.at[way, far - 1, piece],
            device_id={"sp": sides[way]},
            device_id_type=MESH,
        )
        copy.start()
        copies[far, piece, way] = copy

    def close():
        for (far, piece, way), copy in copies.items():
            copy.wait_send()
            if far == half or (far == half - 1 and piece != way):
                copy.wait_recv()

    hops = [
        functools.partial(hop, far, piece, way)
        for far in range(1, half + 1)
        for piece in (0, 1)
        for way in (0, 1)
        if far < half or piece == way
    ]
    return hops, close


def ring_kernel(n, mine, every, send_sem, recv_sem):
    barrier = pltpu.get_barrier_semaphore()
    for side in ring_place(n)[2]:
        pl.semaphore_signal(barrier, inc=1, device_id={"sp": side}, device_id_type=MESH)
    pl.semaphore_wait(barrier, 2)
    hops, close = ring_steps(n, mine, every, send_sem, recv_sem)
    for hop in hops:
        hop()
    every[lax.axis_index("sp")] = mine[...]
    close()


def ring(packed, n):
    return pl.pallas_call(
        functools.partial(ring_kernel, n),
        out_shape=jax.ShapeDtypeStruct((n,) + packed.shape, BF),
        in_specs=[vmem()],
        out_specs=vmem(),
        scratch_shapes=[
            pltpu.SemaphoreType.DMA((2, n // 2, 2)),
            pltpu.SemaphoreType.DMA((2, n // 2, 2)),
        ],
        compiler_params=pltpu.CompilerParams(collective_id=0, has_side_effects=True),
        cost_estimate=pl.CostEstimate(
            flops=30 * 10**9, bytes_accessed=2**20, transcendentals=0
        ),
        name="state_ring",
    )(packed)


def gated(local, carried, state, gate, gain):
    out = local[...].astype(F32) + dot(carried[...], state, NT)
    scale = lax.rsqrt(jnp.mean(jnp.square(out), axis=-1, keepdims=True) + EPS)
    u = gate[...].astype(F32)
    return (out * scale * gain[...] * (u / (1.0 + jnp.exp(-u)))).astype(BF)


def finish_kernel(every, ow, cw, gw, on, cn, gn, gain, weight_w, weight_n, out, total, state):
    wide = cw.shape[1]
    values = ow.shape[1]

    @pl.when(pl.program_id(0) == 0)
    def _():
        total[...] = jnp.zeros_like(total)

        def one(j, carry):
            decay = every[j, values : values + 16, :].astype(F32)[:1]
            total[...] = total[...] * decay + every[j, :values, :].astype(F32)
            return carry

        lax.fori_loop(0, lax.axis_index("sp"), one, 0)
        state[...] = total[...].astype(BF)

    left = gated(ow, cw, state[:, :wide], gw, gain)
    right = gated(on, cn, state[:, wide:], gn, gain)
    out[...] = (dot(left, weight_w[...], NN) + dot(right, weight_n[...], NN)).astype(BF)


def finish(every, ow, cw, gw, on, cn, gn, gain, weight_w, weight_n):
    tokens, values = ow.shape
    rows = min(256, tokens)
    width = weight_w.shape[1]

    def spec(x):
        return pl.BlockSpec((rows, x.shape[1]), lambda i: (i, 0))

    return pl.pallas_call(
        finish_kernel,
        grid=(tokens // rows,),
        in_specs=[vmem()]
        + [spec(x) for x in (ow, cw, gw, on, cn, gn)]
        + [vmem()] * 3,
        out_specs=pl.BlockSpec((rows, width), lambda i: (i, 0)),
        out_shape=jax.ShapeDtypeStruct((tokens, width), BF),
        scratch_shapes=[
            VM((values, every.shape[2]), F32),
            VM((values, every.shape[2]), BF),
        ],
        compiler_params=pltpu.CompilerParams(vmem_limit_bytes=48 * 2**20),
        cost_estimate=pl.CostEstimate(
            flops=20 * 10**9, bytes_accessed=16 * 2**20, transcendentals=0
        ),
        name="finish",
    )(every, ow, cw, gw, on, cn, gn, gain.reshape(1, -1), weight_w, weight_n)


def remote(src, dst, send, recv, to):
    copy = pltpu.make_async_remote_copy(
        src_ref=src, dst_ref=dst, send_sem=send, recv_sem=recv,
        device_id={"tp": to}, device_id_type=MESH,
    )
    copy.start()
    return copy


def greet(t, sides=()):
    barrier = pltpu.get_barrier_semaphore()
    near, far = t + 1 - 2 * lax.rem(t, 2), lax.rem(t + 2, 4)
    for other in (near, far):
        pl.semaphore_signal(barrier, inc=1, device_id={"tp": other}, device_id_type=MESH)
    for side in sides:
        pl.semaphore_signal(barrier, inc=1, device_id={"sp": side}, device_id_type=MESH)
    pl.semaphore_wait(barrier, 2 + len(sides))
    return near, far, lax.rem(near + 2, 4)


def reduce_steps(block, chunks, t, near, far, cross, partial, r1, mix, r2, sems, use):
    s1, v1, s2, v2 = sems
    rows = mix.shape[1]
    sent = []
    for which, owner in ((1, cross), (0, near)):
        for c in range(chunks):
            sent.append(
                (which, c, remote(
                    partial.at[block(owner, c)], r1.at[which, c],
                    s1.at[which, c], v1.at[which, c], near,
                ))
            )
    first = {(w, c): x for w, c, x in sent}
    second = []
    for c in range(chunks):
        first[1, c].wait_recv()
        mix[c] = (partial[block(far, c)].astype(F32) + r1[1, c].astype(F32)).astype(BF)
        second.append(remote(mix.at[c], r2.at[c], s2.at[c], v2.at[c], far))
    for c in range(chunks):
        first[0, c].wait_recv()
        second[c].wait_recv()
        use(c, partial[block(t, c)].astype(F32) + r1[0, c].astype(F32) + r2[c].astype(F32))
    return [x for _, _, x in sent] + second


def mix_kernel(
    n, chunks, partial, residual, gain, shard, stream, normed, weight,
    r1, mix, r2, s1, v1, s2, v2, sx, vx, sn, vn, sf, vf, sw, vw,
):
    t = lax.axis_index("tp")
    near, far, cross = greet(t, ring_place(n)[2])
    hops, close = ring_steps(n, shard, weight, sw, vw)
    first = [hop for hop in hops if hop.args[0] == 1]
    later = [hop for hop in hops if hop.args[0] > 1]
    for hop in first:
        hop()
    rows = mix.shape[1]
    own = rows * chunks

    def block(owner, c):
        return pl.ds(pl.multiple_of(owner * own + c * rows, rows), rows), slice(None)

    def norm(where):
        x = stream[where].astype(F32)
        scale = lax.rsqrt(jnp.mean(jnp.square(x), axis=1, keepdims=True) + EPS)
        normed[where] = (x * scale * gain[...]).astype(BF)

    across, beside, relayed = [], [], []

    def use(c, value):
        where = block(t, c)
        stream[where] = (residual[pl.ds(c * rows, rows), :].astype(F32) + value).astype(BF)
        across.append(remote(stream.at[where], stream.at[where], sx.at[c], vx.at[c], far))
        beside.append(remote(stream.at[where], stream.at[where], sn.at[c], vn.at[c], near))
        for hop in later[2 * c : 2 * c + 2]:
            hop()

    started = reduce_steps(
        block, chunks, t, near, far, cross, partial, r1, mix, r2, (s1, v1, s2, v2), use
    )
    for c in range(chunks):
        norm(block(t, c))
        beside[c].wait_recv()
        norm(block(near, c))
    weight[lax.axis_index("sp")] = shard[...]
    for hop in later[2 * chunks :]:
        hop()
    for c in range(chunks):
        across[c].wait_recv()
        where = block(far, c)
        relayed.append(remote(stream.at[where], stream.at[where], sf.at[c], vf.at[c], near))
        norm(where)
    for c in range(chunks):
        relayed[c].wait_recv()
        norm(block(cross, c))
    for copy in started + across + beside + relayed:
        copy.wait_send()
    close()


def mix_rows(partial, residual, gain, shard, n):
    tokens, width = partial.shape
    chunks = 4
    rows = tokens // 4 // chunks
    dma = pltpu.SemaphoreType.DMA
    return pl.pallas_call(
        functools.partial(mix_kernel, n, chunks),
        out_shape=[jax.ShapeDtypeStruct((tokens, width), BF)] * 2
        + [jax.ShapeDtypeStruct((n,) + shard.shape, BF)],
        in_specs=[vmem()] * 4,
        out_specs=[vmem()] * 3,
        scratch_shapes=[
            VM((2, chunks, rows, width), BF), VM((chunks, rows, width), BF),
            VM((chunks, rows, width), BF),
            dma((2, chunks)), dma((2, chunks)),
        ] + [dma((chunks,))] * 8 + [dma((2, n // 2, 2))] * 2,
        compiler_params=pltpu.CompilerParams(
            collective_id=1, has_side_effects=True, vmem_limit_bytes=48 * 2**20
        ),
        cost_estimate=pl.CostEstimate(
            flops=50 * 10**9, bytes_accessed=16 * 2**20, transcendentals=0
        ),
        name="mix_rows",
    )(partial, residual, gain.reshape(1, -1), shard)


def last_kernel(chunks, partial, stream, out, r1, mix, r2, s1, v1, s2, v2):
    t = lax.axis_index("tp")
    near, far, cross = greet(t)
    rows, width = mix.shape[1:]

    def block(owner, c):
        return pl.ds(c * rows, rows), pl.ds(pl.multiple_of(owner * width, width), width)

    def use(c, value):
        where = pl.ds(c * rows, rows)
        out[where, :] = (stream[where, :].astype(F32) + value).astype(BF)

    for copy in reduce_steps(
        block, chunks, t, near, far, cross, partial, r1, mix, r2, (s1, v1, s2, v2), use
    ):
        copy.wait_send()


def last_columns(partial, stream):
    tokens, width = stream.shape
    chunks = 4
    rows = tokens // chunks
    dma = pltpu.SemaphoreType.DMA
    return pl.pallas_call(
        functools.partial(last_kernel, chunks),
        out_shape=jax.ShapeDtypeStruct((tokens, width), BF),
        in_specs=[vmem()] * 2,
        out_specs=vmem(),
        scratch_shapes=[
            VM((2, chunks, rows, width), BF), VM((chunks, rows, width), BF),
            VM((chunks, rows, width), BF),
            dma((2, chunks)), dma((2, chunks)), dma((chunks,)), dma((chunks,)),
        ],
        compiler_params=pltpu.CompilerParams(
            collective_id=2, has_side_effects=True, vmem_limit_bytes=32 * 2**20
        ),
        name="last_columns",
    )(partial, stream)


def body(
    residual,
    query_wide,
    key_wide,
    value_wide,
    decay_wide,
    gate_wide,
    query_narrow,
    key_narrow,
    value_narrow,
    decay_narrow,
    gate_narrow,
    head_gain,
    out_wide,
    out_narrow,
    mlp_gain,
    up_weight,
    down_weight,
):
    n_sp, n_tp = lax.axis_size("sp"), lax.axis_size("tp")
    assert n_tp == HEADS == 4 and n_sp % 2 == 0
    down_whole = lax.all_gather(down_weight, "sp", axis=1, tiled=True)
    wide_out, wide_q, narrow_out, narrow_q, packed = local_pass(
        query_wide, key_wide, value_wide, decay_wide,
        query_narrow, key_narrow, value_narrow, decay_narrow,
    )
    every = ring(packed, n_sp)
    partial = finish(
        every, wide_out, wide_q, gate_wide, narrow_out, narrow_q, gate_narrow,
        head_gain, out_wide, out_narrow,
    )
    t = lax.axis_index("tp")
    own_rows = residual.shape[0] // n_tp
    own_cols = residual.shape[1] // n_tp
    residual_rows = lax.dynamic_slice_in_dim(residual, t * own_rows, own_rows, 0)
    stream, normed, up_whole = mix_rows(partial, residual_rows, mlp_gain, up_weight, n_sp)
    up_whole = up_whole.reshape(-1, up_weight.shape[1])
    stream_cols = lax.dynamic_slice_in_dim(stream, t * own_cols, own_cols, 1)
    before = jnp.dot(normed, up_whole, preferred_element_type=F32)
    hidden = jnp.square(jax.nn.relu(before)).astype(BF)
    down_terms = jnp.dot(hidden, down_whole, preferred_element_type=F32).astype(BF)
    return last_columns(down_terms, stream_cols)


def solution(mesh):
    return jax.shard_map(
        body,
        mesh=mesh,
        in_specs=(
            P("sp", None),
            P("sp", "tp"),
            P("sp", "tp"),
            P("sp", "tp"),
            P("sp", "tp"),
            P("sp", "tp"),
            P("sp", "tp"),
            P("sp", "tp"),
            P("sp", "tp"),
            P("sp", "tp"),
            P("sp", "tp"),
            P(),
            P("tp", None),
            P("tp", None),
            P(),
            P("sp", "tp"),
            P("tp", "sp"),
        ),
        out_specs=P("sp", "tp"),
        check_vma=False,
    )
```
